32 devices in a mesh: sp: 4 (over z), dp: 8 (over y, x, core).
Axes of the slice: x: 2, y: 2, z: 4, core: 2. Of those that a mesh axis runs over, the one named last changes fastest.
Arguments:
- probe_vectors: bfloat16 [4096, 1024], P(('dp', 'sp')), may hold values from -6 to 6
- address_vectors: bfloat16 [4096, 1024], P(('dp', 'sp')), may hold values from -6 to 6
- content_vectors: bfloat16 [4096, 2048], P(('dp', 'sp')), may hold values from -6 to 6
- adjoint_of_result: bfloat16 [4096, 2048], P(('dp', 'sp')), may hold values from -0.5 to 0.5
- compact_factor: bfloat16 [4096, 64], P(('dp', 'sp')), may hold values from -7.5 to 7.5
- latent_to_damping_map: bfloat16 [64, 1024], replicated, may hold values from -0.75 to 0.75
- damping_shift_term: float32 [1024], replicated
- surplus_damping: bfloat16 [4096, 16], P(('dp', 'sp')), may hold values from -0.7 to 0
Outputs:
- query_grad: bfloat16 [4096, 1024], P(('dp', 'sp'))
- key_grad: bfloat16 [4096, 1024], P(('dp', 'sp'))
- value_grad: bfloat16 [4096, 2048], P(('dp', 'sp'))
- latent_grad: bfloat16 [4096, 64], P(('dp', 'sp'))
- weight_grad: float32 [64, 1024], replicated
The draws below stay inside these ranges and needn't reach their ends.
All inputs are finite; a program needn't handle non-finite values.
Results may differ from the reference program's by a relative error of at most 0.005.
Values may be sent and summed in bfloat16 or wider, within the bound.
No kernel may reach another device: no remote copies, remote signals or barrier semaphores. Data moves between devices by JAX's collectives and lax.ppermute only.
A program may use at most 64 MiB of HBM per device.

```python
import math
import jax
import jax.numpy as jnp
from jax import lax

HEADS = 16
KEY_CHANNELS = 64
VALUE_DIM = 128
RANK = 64
BLOCK = 64
SEQ = 512
TOKENS = 4096
N_DP = 8


def draw_compact_factor(key, part):
    base_key = jax.random.fold_in(key, 11)
    scale_key = jax.random.fold_in(key, 12)
    factor = jnp.exp(jax.random.uniform(scale_key, (TOKENS // BLOCK, 1), jnp.float32, math.log(0.5), math.log(1.5)))
    factor = jnp.repeat(factor, BLOCK, axis=0)
    noise = jnp.clip(jax.random.normal(base_key, (TOKENS, RANK), jnp.float32), -5.0, 5.0)
    return (noise * factor).astype(jnp.bfloat16)


def draw_damping_shift_term(key, part):
    pick_key = jax.random.fold_in(key, 21)
    mixed_key = jax.random.fold_in(key, 22)
    slow_key = jax.random.fold_in(key, 23)
    mixed_count = HEADS // 2
    jitter = 0.5
    ranking = jax.random.permutation(pick_key, HEADS)
    mixed = (ranking < mixed_count)[:, None]
    mixed_value = jax.random.uniform(mixed_key, (HEADS, KEY_CHANNELS), jnp.float32, -3.0, 6.0)
    slow_value = math.log(SEQ / 16.0) + 1.2 + jax.random.uniform(slow_key, (HEADS, KEY_CHANNELS), jnp.float32, -jitter, jitter)
    return jnp.where(mixed, mixed_value, slow_value).reshape(HEADS * KEY_CHANNELS)


def draw_surplus_damping(key, part):
    where_key = jax.random.fold_in(key, 31)
    depth_key = jax.random.fold_in(key, 32)
    hits = jax.random.uniform(where_key, (TOKENS, HEADS), jnp.float32) < 2.0 / SEQ
    depth = jax.random.uniform(depth_key, (TOKENS, HEADS), jnp.float32, math.log(0.5), math.log(0.8))
    return jnp.where(hits, depth, jnp.zeros_like(depth)).astype(jnp.bfloat16)


def level_of(stream_key, dims, pieces, smallest, top_value):
    loudness = 1.0
    for dim, blocks in pieces:
        heights = jax.random.uniform(jax.random.fold_in(jax.random.fold_in(stream_key, 6), dim), (blocks,), jnp.float32, smallest / len(pieces), top_value / len(pieces))
        loudness = loudness * jnp.repeat(jnp.exp(heights), dims[dim] // blocks).reshape((-1,) + (1,) * (len(dims) - 1 - dim))
    return loudness


def centred(key, dims, spread, reach, shards=(), kind=jnp.bfloat16):
    result = jax.random.normal(key, dims, jnp.float32) * spread
    if len(shards) > 0:
        result = level_of(key, dims, shards, -0.22, 0.18) * result
    return jnp.clip(result, min=-reach, max=reach).astype(kind)


def setup_inputs(seed: int = 0) -> dict:
    splits = jax.random.split(jax.random.key(seed), 9)
    probe_vectors = centred(splits[0], (TOKENS, HEADS * KEY_CHANNELS), 1.0, 6.0, ((0, 32),))
    address_vectors = centred(splits[1], (TOKENS, HEADS * KEY_CHANNELS), 1.0, 6.0, ((0, 32),))
    content_vectors = centred(splits[2], (TOKENS, HEADS * VALUE_DIM), 1.0, 6.0, ((0, 32),))
    adjoint_of_result = centred(splits[3], (TOKENS, HEADS * VALUE_DIM), (8 * (SEQ * VALUE_DIM) ** -0.5), 0.5, ((0, 32),))
    compact_factor = draw_compact_factor(jax.random.fold_in(splits[8], 71), 0)
    latent_to_damping_map = centred(splits[5], (RANK, HEADS * KEY_CHANNELS), RANK ** -0.5, 0.75)
    damping_shift_term = draw_damping_shift_term(jax.random.fold_in(splits[8], 71), 0)
    surplus_damping = draw_surplus_damping(jax.random.fold_in(splits[8], 71), 0)
    return {"probe_vectors": probe_vectors, "address_vectors": address_vectors, "content_vectors": content_vectors, "adjoint_of_result": adjoint_of_result, "compact_factor": compact_factor, "latent_to_damping_map": latent_to_damping_map, "damping_shift_term": damping_shift_term, "surplus_damping": surplus_damping}


gate_norm = 16.0
highest = lax.Precision.HIGHEST

def carry_states(block_total, increments):
    log_totals = block_total[:, :, 0, :]
    running = jnp.cumsum(log_totals, axis=1)
    before = running - log_totals
    blocks = log_totals.shape[1]
    order = jnp.arange(blocks, dtype=jnp.int32)
    earlier_mask = (order[None, :] < order[:, None])[None, :, :, None]
    exponent = before[:, :, None, :] - running[:, None, :, :]
    exponent = jnp.where(earlier_mask, exponent, jnp.zeros_like(exponent))
    weights = jnp.where(earlier_mask, jnp.exp(exponent), jnp.zeros_like(exponent))
    return jnp.einsum('hnmk,mhkv->nhkv', weights, increments, precision=highest)

def gla_forward(probe_vectors, address_vectors, content_vectors, logarithm_decay):
    head_count, seq_len, key_width = probe_vectors.shape
    value_width = content_vectors.shape[2]
    blocks = seq_len // BLOCK

    def blocked(tensor):
        return tensor.reshape(head_count, blocks, BLOCK, tensor.shape[2])
    cumulative = jnp.cumsum(blocked(logarithm_decay), axis=2)
    block_total = cumulative[:, :, BLOCK - 1:, :]
    keys_block = blocked(address_vectors)
    query_decayed = blocked(probe_vectors) * key_width ** (-0.5) * jnp.exp(cumulative)
    key_inverse = keys_block * jnp.exp(-cumulative)
    key_to_end = keys_block * jnp.exp(block_total - cumulative)
    value_block = blocked(content_vectors)
    scores = jnp.einsum('hnik,hnjk->hnij', query_decayed, key_inverse, precision=highest)
    positions = jnp.arange(BLOCK, dtype=jnp.int32)
    causal = positions[:, None] >= positions[None, :]
    scores = jnp.where(causal, scores, jnp.zeros_like(scores))
    within_block = jnp.einsum('hnij,hnjv->hniv', scores, value_block, precision=highest)
    increments = jnp.einsum('hnjk,hnjv->nhkv', key_to_end, value_block, precision=highest)
    earlier = carry_states(block_total, increments)
    carried = jnp.einsum('hnik,nhkv->hniv', query_decayed, earlier, precision=highest)
    return (within_block + carried).reshape(head_count, seq_len, value_width)

def split_into_heads(tensor, width):
    return tensor.astype(jnp.float32).reshape(SEQ, HEADS, width).transpose(1, 0, 2)

def to_rows(tensor):
    return tensor.transpose(1, 0, 2).reshape(SEQ, tensor.shape[0] * tensor.shape[2])

def stream_array_group(tensor):
    return tensor.reshape(N_DP, SEQ, tensor.shape[1])

def flatten(tensor):
    return tensor.reshape(TOKENS, tensor.shape[2])

def reference(probe_vectors, address_vectors, content_vectors, adjoint_of_result, compact_factor, latent_to_damping_map, damping_shift_term, surplus_damping):

    def lone_stream(input_bundle):
        query_token_rows, key_token_rows, value_token_rows, upstream_rows, hidden_code_rows, spike_rows = input_bundle
        gate_logit = jnp.dot(hidden_code_rows, latent_to_damping_map, preferred_element_type=jnp.float32) + damping_shift_term
        logarithm_decay = split_into_heads(jax.nn.log_sigmoid(gate_logit) / gate_norm, KEY_CHANNELS)
        logarithm_decay = logarithm_decay + spike_rows.astype(jnp.float32).T[:, :, None]
        _, pullback = jax.vjp(gla_forward, split_into_heads(query_token_rows, KEY_CHANNELS), split_into_heads(key_token_rows, KEY_CHANNELS), split_into_heads(value_token_rows, VALUE_DIM), logarithm_decay)
        grad_query, grad_key, grad_value, grad_decay = pullback(split_into_heads(upstream_rows, VALUE_DIM))
        gate_grad = (to_rows(grad_decay) * jax.nn.sigmoid(-gate_logit) / gate_norm).astype(jnp.bfloat16)
        latent_part = jnp.dot(gate_grad, latent_to_damping_map.T, preferred_element_type=jnp.float32).astype(jnp.bfloat16)
        weight_term = jnp.dot(hidden_code_rows.T, gate_grad, preferred_element_type=jnp.float32)
        return (to_rows(grad_query).astype(jnp.bfloat16), to_rows(grad_key).astype(jnp.bfloat16), to_rows(grad_value).astype(jnp.bfloat16), latent_part, weight_term)
    returned_results = lax.map(lone_stream, (stream_array_group(probe_vectors), stream_array_group(address_vectors), stream_array_group(content_vectors), stream_array_group(adjoint_of_result), stream_array_group(compact_factor), stream_array_group(surplus_damping)))
    weight_grad = lax.optimization_barrier(jnp.sum(returned_results[4], axis=0))
    return (flatten(returned_results[0]), flatten(returned_results[1]), flatten(returned_results[2]), flatten(returned_results[3]), weight_grad)
```

```python
import functools

import jax
import jax.numpy as jnp
from jax import lax
from jax.experimental import pallas as pl
from jax.experimental.pallas import tpu as pltpu
from jax.sharding import PartitionSpec as P

KEY = 64
VAL = 128
LANES = 128
BLOCK = 64
GATE_NORM = 16.0
SCALE = KEY ** (-0.5)
F32 = jnp.float32
BF16 = jnp.bfloat16

NN = (((1,), (0,)), ((), ()))
NT = (((1,), (1,)), ((), ()))
TN = (((0,), (0,)), ((), ()))


def dot(a, b, dims=NN):
    return lax.dot_general(a, b, dims, preferred_element_type=F32)


def split(x, parts):
    pieces = []
    for _ in range(parts):
        piece = x.astype(BF16)
        pieces.append(piece)
        x = x - piece.astype(F32)
    return pieces


def triangle(rows, keep):
    r = lax.broadcasted_iota(jnp.int32, (rows, rows), 0)
    c = lax.broadcasted_iota(jnp.int32, (rows, rows), 1)
    return jnp.where(keep(r, c), 1.0, 0.0).astype(BF16)


def first_head(shape):
    return lax.broadcasted_iota(jnp.int32, shape, 1) < KEY


def pick(a, b):
    return jnp.where(first_head(a.shape), a, b)


def lanes(p):
    return slice(p * LANES, (p + 1) * LANES)


def value_lanes(h):
    return slice(h * VAL, (h + 1) * VAL)


def gates_kernel(q, k, v, do, c, w, b, spike, st, rt, cum_ref, sig_ref, qs_ref, kd_ref):
    rows, width = q.shape
    heads = spike.shape[1]
    logit = dot(c[...], w[...]) + b[...]
    small = jnp.exp(-jnp.abs(logit))
    log_sig = jnp.minimum(logit, 0.0) - jnp.log1p(small)
    sig_ref[...] = jnp.where(logit >= 0.0, small, 1.0) / ((1.0 + small) * GATE_NORM)
    owner = lax.broadcasted_iota(jnp.int32, (heads, width), 1) // KEY
    head = lax.broadcasted_iota(jnp.int32, (heads, width), 0)
    spread = jnp.where(owner == head, 1.0, 0.0).astype(BF16)
    log_decay = log_sig / GATE_NORM + dot(spike[...], spread)
    lower = triangle(rows, lambda r, s: r >= s)
    cum = sum(dot(lower, piece) for piece in split(log_decay, 3))
    cum_ref[...] = cum
    total = cum[rows - 1 :, :]
    qs = (q[...].astype(F32) * (SCALE * jnp.exp(cum))).astype(BF16)
    kd = (k[...].astype(F32) * jnp.exp(total - cum)).astype(BF16)
    qs_ref[...] = qs
    kd_ref[...] = kd
    for p in range(width // LANES):
        both = slice(2 * p * VAL, 2 * (p + 1) * VAL)
        s_pair = dot(v[:, both], kd[:, lanes(p)], TN)
        st[:, lanes(p)] = pick(s_pair[:VAL], s_pair[VAL:]).astype(BF16)
        r_pair = dot(do[:, both], qs[:, lanes(p)], TN)
        rt[:, lanes(p)] = pick(r_pair[:VAL], r_pair[VAL:]).astype(BF16)


def inner_kernel(q, k, v, do, cum_ref, dq, dk, dv, dec):
    rows, width = q.shape
    upper = triangle(rows, lambda r, s: r <= s)
    r = lax.broadcasted_iota(jnp.int32, (rows, rows), 0)
    s = lax.broadcasted_iota(jnp.int32, (rows, rows), 1)
    causal = r >= s
    causal_t = r <= s
    for p in range(width // LANES):
        cum = cum_ref[:, lanes(p)]
        middle = cum[BLOCK - 1 : BLOCK, :]
        q_up = SCALE * jnp.exp(cum - middle)
        k_up = jnp.exp(middle - cum)
        qa = (q[:, lanes(p)].astype(F32) * q_up).astype(BF16)
        ka = (k[:, lanes(p)].astype(F32) * k_up).astype(BF16)
        zero = jnp.zeros_like(ka)
        grads = []
        for j in range(2):
            h = 2 * p + j
            own = first_head(ka.shape) if j == 0 else jnp.logical_not(first_head(ka.shape))
            vj = v[:, value_lanes(h)]
            doj = do[:, value_lanes(h)]
            at = jnp.where(causal_t, dot(jnp.where(own, ka, zero), qa, NT), 0.0).astype(BF16)
            dv[:, value_lanes(h)] = dot(at, doj)
            g = jnp.where(causal, dot(doj, vj, NT), 0.0).astype(BF16)
            gt = jnp.where(causal_t, dot(vj, doj, NT), 0.0).astype(BF16)
            grads.append((dot(g, ka), dot(gt, qa)))
        dqa = pick(grads[0][0], grads[1][0])
        dka = pick(grads[0][1], grads[1][1])
        dq[:, lanes(p)] = dqa * q_up
        dk[:, lanes(p)] = dka * k_up
        flow = qa.astype(F32) * dqa - ka.astype(F32) * dka
        dec[:, lanes(p)] = sum(dot(upper, piece) for piece in split(flow, 3))


def carried(x, state, p):
    return pick(
        dot(x[:, value_lanes(2 * p)], state[:, lanes(p)]),
        dot(x[:, value_lanes(2 * p + 1)], state[:, lanes(p)]),
    )


def weight_kernel(v, do, c, cum_ref, sig_ref, qs, kd, dec, st, rt, gate, wg):
    rows, width = qs.shape
    upper = triangle(rows, lambda r, s: r <= s)
    before = triangle(rows, lambda r, s: r > s)
    for p in range(width // LANES):
        sp, rp = st[:, lanes(p)], rt[:, lanes(p)]
        t2 = qs[:, lanes(p)].astype(F32) * carried(do, st, p)
        t3 = kd[:, lanes(p)].astype(F32) * carried(v, rt, p)
        meet = jnp.sum(sp.astype(F32) * rp.astype(F32), axis=0, keepdims=True)
        total = jnp.exp(cum_ref[rows - 1 :, lanes(p)]) * meet + dec[:, lanes(p)]
        total += sum(dot(upper, piece) for piece in split(t2, 3))
        total += sum(dot(before, piece) for piece in split(t3, 3))
        g = (total * sig_ref[:, lanes(p)]).astype(BF16)
        gate[:, lanes(p)] = g
        wg[:, lanes(p)] = dot(c[...], g, TN)


def finish_kernel(v, do, w, cum_ref, kd, dq_in, dk_in, dv_in, st, rt, gate, dq, dk, dv, lat):
    rows, width = kd.shape
    lat[...] = dot(gate[...], w[...], NT).astype(BF16)
    for p in range(width // LANES):
        cum = cum_ref[:, lanes(p)]
        total = cum[rows - 1 :, :]
        dq[:, lanes(p)] = (
            dq_in[:, lanes(p)] + carried(do, st, p) * (SCALE * jnp.exp(cum))
        ).astype(BF16)
        dk[:, lanes(p)] = (
            dk_in[:, lanes(p)] + carried(v, rt, p) * jnp.exp(total - cum)
        ).astype(BF16)
        kp = kd[:, lanes(p)]
        zero = jnp.zeros_like(kp)
        for j in range(2):
            h = 2 * p + j
            own = first_head(kp.shape) if j == 0 else jnp.logical_not(first_head(kp.shape))
            add = dot(jnp.where(own, kp, zero), rt[:, lanes(p)], NT)
            dv[:, value_lanes(h)] = (dv_in[:, value_lanes(h)] + add).astype(BF16)


def call(kernel, outs, flops, *args):
    moved = sum(a.size * a.dtype.itemsize for a in args)
    return pl.pallas_call(
        kernel,
        out_shape=[jax.ShapeDtypeStruct(s, d) for s, d in outs],
        compiler_params=pltpu.CompilerParams(vmem_limit_bytes=24 * 1024 * 1024),
        cost_estimate=pl.CostEstimate(flops=flops, bytes_accessed=moved, transcendentals=0),
        name=kernel.__name__,
    )(*args)


def swap(x, axis, size, bit):
    return lax.ppermute(x, axis, [(i, i ^ bit) for i in range(size)])


def add_over(x, axis, size, low):
    bit = low
    while bit < size:
        x = x.astype(BF16)
        if 2 * bit < size:
            one, two, three = (swap(x, axis, size, m * bit) for m in (1, 2, 3))
            x = (x.astype(F32) + one.astype(F32)) + (two.astype(F32) + three.astype(F32))
            bit *= 4
        else:
            x = x.astype(F32) + swap(x, axis, size, bit).astype(F32)
            bit *= 2
    return x


def exchange(st, rt, decay, n, ndp):
    me = lax.axis_index("sp")
    left = jnp.zeros_like(st)
    right = jnp.zeros_like(rt)
    for step in range(n - 1):
        mirror = n - 1 - step
        forward = st.astype(F32) + decay * left.astype(F32)
        backward = rt.astype(F32) + decay * right.astype(F32)
        message = jnp.where(me == step, forward, backward).astype(BF16)
        partner = {}
        for a, b in ((step, step + 1), (mirror, mirror - 1)):
            partner[a] = b
        for a, b in list(partner.items()):
            partner.setdefault(b, a)
        whole = all(partner.get(b) == a for a, b in partner.items())
        pairs = []
        for i in range(n):
            for d in range(ndp):
                if i in partner:
                    pairs.append((i * ndp + d, partner[i] * ndp + d))
                elif ndp % 2 == 0:
                    pairs.append((i * ndp + d, i * ndp + (d ^ 1)))
        if not whole:
            pairs = [
                (a * ndp + d, b * ndp + d)
                for a, b in ((step, step + 1), (mirror, mirror - 1))
                for d in range(ndp)
            ]
        got = lax.ppermute(message, ("sp", "dp"), pairs)
        left = jnp.where(me == step + 1, got, left)
        right = jnp.where(me == mirror - 1, got, right)
    return left, right


def on_device(n, ndp, q, k, v, do, c, w, b, spike):
    rows, width = q.shape
    rank = c.shape[1]
    wide = v.shape[1]
    square = 2 * rows * wide * rows
    st, rt, cum, sig, qs, kd = call(
        gates_kernel,
        [((VAL, width), BF16)] * 2
        + [((rows, width), F32)] * 2
        + [((rows, width), BF16)] * 2,
        2 * square,
        q, k, v, do, c, w, b.reshape(1, width), spike,
    )
    dq_in, dk_in, dv_in, dec = call(
        inner_kernel,
        [((rows, width), F32)] * 2 + [((rows, wide), F32), ((rows, width), F32)],
        6 * square,
        q, k, v, do, cum,
    )
    decay = jnp.exp(cum[rows - 1 :, :])
    left, right = exchange(st, rt, decay, n, ndp)
    gate, part = call(
        weight_kernel,
        [((rows, width), BF16), ((rank, width), F32)],
        3 * square,
        v, do, c, cum, sig, qs, kd, dec, left, right,
    )
    dq, dk, dv, lat = call(
        finish_kernel,
        [((rows, width), BF16)] * 2 + [((rows, wide), BF16), ((rows, rank), BF16)],
        4 * square,
        v, do, w, cum, kd, dq_in, dk_in, dv_in, left, right, gate,
    )
    half = rank // 2
    odd = lax.axis_index("dp") % 2 == 1
    mine = jnp.where(odd, part[half:], part[:half])
    other = jnp.where(odd, part[:half], part[half:])
    mine = mine + swap(other, "dp", ndp, 1)
    mine = add_over(mine, "dp", ndp, 2)
    mine = add_over(mine, "sp", n, 1)
    other = swap(mine, "dp", ndp, 1)
    weight = jnp.concatenate([jnp.where(odd, other, mine), jnp.where(odd, mine, other)], axis=0)
    return dq, dk, dv, lat, weight


def solution(mesh):
    token = P(("dp", "sp"), None)
    return jax.shard_map(
        functools.partial(on_device, mesh.shape["sp"], mesh.shape["dp"]),
        mesh=mesh,
        in_specs=(token, token, token, token, token, P(), P(), token),
        out_specs=(token, token, token, token, P()),
        check_vma=False,
    )
```
